32 devices in a mesh: sp: 8 (over z, x), tp: 4 (over y, core).
Axes of the slice: x: 2, y: 2, z: 4, core: 2. Of those that a mesh axis runs over, the one named last changes fastest.
Arguments:
- tokens: bfloat16 [1536, 2048], P(('sp', 'tp')), may hold values from -54 to 54
- w_query: bfloat16 [2048, 2048], P(None, 'tp'), may hold values from -0.21875 to 0.21875
- w_key: bfloat16 [2048, 2048], P(None, 'tp'), may hold values from -0.125 to 0.125
- w_value: bfloat16 [2048, 2048], P(None, 'tp'), may hold values from -0.125 to 0.125
- w_out: bfloat16 [2048, 2048], P('tp'), may hold values from -0.125 to 0.125
- mix_weight: float32 [16], P('tp'), may hold values from 0.3 to 0.8
- out_gain: float32 [128], replicated, may hold values from 0.1 to 1.9
Outputs:
- mixed: bfloat16 [1536, 2048], P(('sp', 'tp'))
The draws below stay inside these ranges and needn't reach their ends.
All inputs are finite; a program needn't handle non-finite values.
Results may differ from the reference program's by a relative error of at most 0.018.
The reference program's roundings to bfloat16 on the way (of `queries`, `keys`, `values`, `weights` and `normed`) count: a program that leaves them out, or rounds other values in their place, can miss the bound.
Values may be sent and summed in bfloat16 or wider, within the bound.
A program may use at most 192 MiB of HBM per device.

```python
import math
import jax
import jax.numpy as jnp
from jax import lax

D = 2048
HEADS = 16
HD = 64
VD = 128
TOKENS = 1536


def draw_tokens(key, part):
    key_noise = jax.random.fold_in(key, 11)
    key_dir = jax.random.fold_in(key, 12)
    noise = jax.random.truncated_normal(key_noise, -6.0, 6.0, (TOKENS, D), jnp.float32)
    direction = jax.random.truncated_normal(key_dir, -6.0, 6.0, (D,), jnp.float32)
    place = jnp.arange(TOKENS, dtype=jnp.float32) / TOKENS
    drift = jnp.cos(3.14159265 * place)
    result = noise + drift[:, None] * direction[None, :]
    return result.astype(jnp.bfloat16)


def level_of(rng, shape, pieces, least, high):
    def one(position, shards_of):
        draws = jax.random.uniform(jax.random.fold_in(jax.random.fold_in(rng, 6), position), (shards_of,), jnp.float32, least / len(pieces), high / len(pieces))
        return jnp.repeat(jnp.exp(draws), shape[position] // shards_of).reshape((-1,) + (1,) * (len(shape) - position - 1))

    loudness = one(*pieces[0])
    for cut in pieces[1:]:
        loudness = loudness * one(*cut)
    return loudness


def gaussian(own_key, dims, deviation, reach, shards=(), held_as=jnp.bfloat16):
    values = jax.random.normal(own_key, dims, jnp.float32) * deviation
    if len(shards) > 0:
        values = level_of(own_key, dims, shards, -0.22, 0.18) * values
    return jnp.clip(values, min=-reach, max=reach).astype(held_as)


def setup_inputs(seed: int = 0) -> dict:
    seeds = jax.random.split(jax.random.key(seed), 8)
    tokens = draw_tokens(jax.random.fold_in(seeds[7], 71), 0)
    w_query = gaussian(seeds[1], (D, HEADS * 2 * HD), (D // 3) ** -0.5, 0.21875, ((1, 4),))
    w_key = gaussian(seeds[2], (D, HEADS * 2 * HD), D ** -0.5, 0.125, ((1, 4),))
    w_value = gaussian(seeds[3], (D, HEADS * VD), D ** -0.5, 0.125, ((1, 4),))
    w_out = gaussian(seeds[4], (HEADS * VD, D), (HEADS * VD) ** -0.5, 0.125, ((0, 4),))
    mix_weight = jnp.clip(0.3 + 0.5 * jax.random.uniform(seeds[5], (HEADS,), jnp.float32) ** level_of(seeds[5], (HEADS,), ((0, 4),), -0.2, 0.2), 0.3, 0.8)
    out_gain = jnp.clip(1.0 + 0.18 * jax.random.normal(seeds[6], (VD,), jnp.float32), 0.1, 1.9)
    return dict(tokens=tokens, w_query=w_query, w_key=w_key, w_value=w_value, w_out=w_out, mix_weight=mix_weight, out_gain=out_gain)


def one_head(args):
    query_h, key_h, value_h, lam = args
    block = math.gcd(TOKENS, 1024)
    query_blocks = query_h.reshape(TOKENS // block, block, 2, HD)
    key_f = key_h.astype(jnp.float32)
    value_f = value_h.astype(jnp.float32)

    def per_block(query_b):
        scores = jnp.einsum('qmd,kmd->mqk', query_b.astype(jnp.float32), key_f) * HD ** (-0.5)
        top = lax.optimization_barrier(jnp.max(scores, axis=-1, keepdims=True))
        expw = jnp.exp(scores - top)
        total = lax.optimization_barrier(jnp.sum(expw, axis=-1))
        weights = expw.astype(jnp.bfloat16).astype(jnp.float32)
        accum = jnp.einsum('mqk,ke->mqe', weights, value_f)
        return accum[0] / total[0][:, None] - lam * accum[1] / total[1][:, None]
    return lax.map(per_block, query_blocks).reshape(TOKENS, VD)

def reference(tokens, w_query, w_key, w_value, w_out, mix_weight, out_gain):
    queries = jnp.dot(tokens, w_query, preferred_element_type=jnp.float32).astype(jnp.bfloat16)
    keys = jnp.dot(tokens, w_key, preferred_element_type=jnp.float32).astype(jnp.bfloat16)
    values = jnp.dot(tokens, w_value, preferred_element_type=jnp.float32).astype(jnp.bfloat16)
    query_h = queries.reshape(TOKENS, HEADS, 2, HD).transpose(1, 0, 2, 3)
    key_h = keys.reshape(TOKENS, HEADS, 2, HD).transpose(1, 0, 2, 3)
    value_h = values.reshape(TOKENS, HEADS, VD).transpose(1, 0, 2)
    heads_out = lax.map(one_head, (query_h, key_h, value_h, mix_weight))
    meansq = lax.optimization_barrier(jnp.mean(heads_out * heads_out, axis=-1, keepdims=True))
    normed = (heads_out * lax.rsqrt(meansq + 1e-06) * out_gain).astype(jnp.bfloat16)
    normed = normed.transpose(1, 0, 2).reshape(TOKENS, HEADS * VD)
    return jnp.dot(normed, w_out, preferred_element_type=jnp.float32).astype(jnp.bfloat16)
```

```python
import functools
import math

import jax
import jax.numpy as jnp
from jax import lax
from jax.experimental import pallas as pl
from jax.experimental.pallas import tpu as pltpu
from jax.sharding import PartitionSpec as P


def block_rows(rows):
    best = 1
    for candidate in range(1, rows + 1):
        if rows % candidate == 0 and candidate <= 2048:
            best = candidate
    return best


def shards(tokens, w_query, w_key, w_value, w_out, mix_weight, out_gain):
    query_cols = w_query.shape[1]
    key_cols = w_key.shape[1]
    heads_here = mix_weight.shape[0]
    head_dim = query_cols // (2 * heads_here)
    value_dim = w_value.shape[1] // heads_here
    piece = lax.all_gather(tokens, "tp", axis=0, tiled=True)
    part_q = jnp.dot(piece, w_query, preferred_element_type=jnp.float32).astype(jnp.bfloat16)
    part_k = jnp.dot(piece, w_key, preferred_element_type=jnp.float32).astype(jnp.bfloat16)
    part_v = jnp.dot(piece, w_value, preferred_element_type=jnp.float32).astype(jnp.bfloat16)
    joined = jnp.concatenate([part_q, part_k, part_v], axis=1)
    queries = joined[:, :query_cols]
    keys = joined[:, query_cols : query_cols + key_cols]
    values = joined[:, query_cols + key_cols :]
    n_query = queries.shape[0]
    query_four = queries.reshape(n_query, heads_here, 2, head_dim)
    scale = head_dim ** (-0.5)

    def step(carry, block):
        running_max, running_sum, accum = carry
        key_blk, value_blk = block
        scores = (
            jnp.einsum("qhmd,khmd->hmqk", query_four, key_blk, preferred_element_type=jnp.float32)
            * scale
        )
        new_max = jnp.maximum(running_max, jnp.max(scores, axis=-1))
        factor = jnp.exp(running_max - new_max)
        expw = jnp.exp(scores - new_max[..., None])
        running_sum = running_sum * factor + jnp.sum(expw, axis=-1)
        weights = expw.astype(jnp.bfloat16)
        accum = accum * factor[..., None] + jnp.einsum(
            "hmqk,khe->hmqe", weights, value_blk, preferred_element_type=jnp.float32
        )
        return ((new_max, running_sum, accum), None)

    initial = (
        jnp.full((heads_here, 2, n_query), -1e30, jnp.float32),
        jnp.zeros((heads_here, 2, n_query), jnp.float32),
        jnp.zeros((heads_here, 2, n_query, value_dim), jnp.float32),
    )
    all_keys, all_values = (
        lax.all_gather(keys, "sp", axis=0, tiled=True),
        lax.all_gather(values, "sp", axis=0, tiled=True),
    )
    carry = initial
    rows = all_keys.shape[0]
    group = block_rows(rows)
    key_blocks = all_keys.reshape(rows // group, group, heads_here, 2, head_dim)
    value_blocks = all_values.reshape(rows // group, group, heads_here, value_dim)
    carry, unused = lax.scan(step, carry, (key_blocks, value_blocks))
    running_max, running_sum, accum = carry
    heads_out = (
        accum[:, 0] / running_sum[:, 0, :, None]
        - mix_weight[:, None, None] * accum[:, 1] / running_sum[:, 1, :, None]
    )
    meansq = jnp.mean(heads_out * heads_out, axis=-1, keepdims=True)
    normed = (heads_out * lax.rsqrt(meansq + 1e-06) * out_gain).astype(jnp.bfloat16)
    normed = normed.transpose(1, 0, 2).reshape(n_query, heads_here * value_dim)
    return lax.psum_scatter(
        jnp.dot(normed, w_out, preferred_element_type=jnp.float32).astype(jnp.bfloat16),
        "tp",
        scatter_dimension=0,
        tiled=True,
    )


BF16 = jnp.bfloat16
F32 = jnp.float32
MESH = pl.DeviceIdType.MESH
CHUNKS = 4


def remote(src, dst, send, recv, where):
    return pltpu.make_async_remote_copy(
        src_ref=src, dst_ref=dst, send_sem=send, recv_sem=recv, device_id=where, device_id_type=MESH
    )


def kernel(
    nh, mix_ref, gain_ref, tok_ref, wq_hbm, wk_hbm, wv_hbm, wo_hbm, out_ref,
    wq, wk, wv, wo, tok, snd, rcv, kvx, nsnd, nrm, keep, dsnd, drcv, ysnd, yrcv,
    w_sem, a_ss, a_rs, z_ss, z_rs, x_ss, x_rs, c_ss, c_rs, d_ss, d_rs, y_ss, y_rs,
):
    rows, width = tok_ref.shape
    pair = 2 * rows
    block = 2 * pair
    vd = gain_ref.shape[1]
    s, t = lax.axis_index("sp"), lax.axis_index("tp")
    h, g = s // 2, s % 2
    core_peer = {"tp": t + 1 - 2 * (t % 2)}
    row_peer = {"tp": t + 2 - 4 * (t // 2)}
    side_peer = {"sp": h * 2 + (1 - g)}

    def head_peer(d):
        return {"sp": lax.rem(h + d, nh) * 2 + g}

    loads = [
        pltpu.make_async_copy(a, b, w_sem.at[i])
        for i, (a, b) in enumerate(((wq_hbm, wq), (wk_hbm, wk), (wv_hbm, wv), (wo_hbm, wo)))
    ]
    for load in loads:
        load.start()

    barrier = pltpu.get_barrier_semaphore()
    peers = [core_peer, row_peer, side_peer] + [head_peer(d) for d in range(1, nh)]
    for peer in peers:
        pl.semaphore_signal(barrier, inc=1, device_id=peer, device_id_type=MESH)
    pl.semaphore_wait(barrier, len(peers))

    pending = []
    to_row = remote(tok_ref, tok.at[1], a_ss.at[1], a_rs.at[1], row_peer)
    to_row.start()
    to_core = remote(tok_ref, tok.at[0], a_ss.at[0], a_rs.at[0], core_peer)
    to_core.start()
    forward = remote(tok.at[1], tok.at[2], a_ss.at[2], a_rs.at[2], core_peer)
    pending += [to_row, to_core, forward]

    z_copies, x_copies = {}, {}

    def project(p, x):
        at = pl.ds(p * pair, pair)
        for i, w in enumerate((wq, wk, wv)):
            if p == 0:
                loads[i].wait()
            y = jnp.dot(x, w[...], preferred_element_type=F32).astype(BF16)
            for hh in range(nh):
                snd[hh, i, at, :] = y[:, hh * vd : (hh + 1) * vd]
        for d in range(1, nh):
            z_copies[p, d] = remote(
                snd.at[lax.rem(h + d, nh), :, at, :],
                rcv.at[:, pl.ds(d * block + p * pair, pair), :],
                z_ss.at[p, d - 1],
                z_rs.at[p, d - 1],
                head_peer(d),
            )
            z_copies[p, d].start()
        x_copies[p, 0] = remote(
            snd.at[h, pl.ds(1, 2), at, :], kvx.at[:, at, :], x_ss.at[p, 0], x_rs.at[p, 0], side_peer
        )
        x_copies[p, 0].start()
        rcv[:, at, :] = snd[h, :, at, :]

    def relay(p, d):
        z_copies[p, d].wait_recv()
        at = pl.ds(d * block + p * pair, pair)
        x_copies[p, d] = remote(
            rcv.at[pl.ds(1, 2), at, :], kvx.at[:, at, :], x_ss.at[p, d], x_rs.at[p, d], side_peer
        )
        x_copies[p, d].start()

    to_core.wait_recv()
    project(0, jnp.concatenate([tok_ref[...], tok[0]], axis=0))
    to_row.wait_recv()
    forward.start()
    forward.wait_recv()
    project(1, tok[1:3].reshape(pair, width))
    for p in range(2):
        for d in range(1, nh):
            relay(p, d)
    for p in range(2):
        for d in range(nh):
            x_copies[p, d].wait_recv()

    pending += list(z_copies.values()) + list(x_copies.values())

    hd = vd // 2
    c = (hd ** -0.5) * math.log2(math.e)
    lam = mix_ref[h]
    gain = gain_ref[...]
    lane = lax.broadcasted_iota(jnp.int32, (block, vd), 1)
    c_copies = []
    nt = (((1,), (1,)), ((), ()))
    for d in list(range(1, nh)) + [0]:
        q = rcv[0, pl.ds(d * block, block), :]
        zero = jnp.zeros_like(q)
        qq = jnp.concatenate([jnp.where(lane < hd, q, zero), jnp.where(lane < hd, zero, q)], axis=0)
        s0 = lax.dot_general(qq, rcv[1], nt, preferred_element_type=F32)
        s1 = lax.dot_general(qq, kvx[0], nt, preferred_element_type=F32)
        top = jnp.maximum(jnp.max(s0, axis=1, keepdims=True), jnp.max(s1, axis=1, keepdims=True))
        e0 = jnp.exp2((s0 - top) * c)
        e1 = jnp.exp2((s1 - top) * c)
        total = jnp.sum(e0, axis=1, keepdims=True) + jnp.sum(e1, axis=1, keepdims=True)
        acc = jnp.dot(e0.astype(BF16), rcv[2], preferred_element_type=F32)
        acc = acc + jnp.dot(e1.astype(BF16), kvx[1], preferred_element_type=F32)
        o = acc / total
        o = o[:block] - lam * o[block:]
        meansq = jnp.mean(o * o, axis=1, keepdims=True)
        normed = (o * lax.rsqrt(meansq + 1e-06) * gain).astype(BF16)
        if d == 0:
            nrm[h] = normed
        else:
            nsnd[d - 1] = normed
            back = remote(
                nsnd.at[d - 1], nrm.at[h], c_ss.at[d - 1], c_rs.at[d - 1], head_peer(nh - d)
            )
            back.start()
            c_copies.append(back)
    for back in c_copies:
        back.wait_recv()
    pending += c_copies

    loads[3].wait()
    n = jnp.concatenate([nrm[i] for i in range(nh)], axis=1)
    step = width // CHUNKS
    d_copies, y_copies = [], []
    for k in range(CHUNKS):
        part = jnp.dot(n, wo[:, k * step : (k + 1) * step], preferred_element_type=F32)
        dsnd[k, 0] = part[rows : 2 * rows].astype(BF16)
        dsnd[k, 1] = part[3 * rows :].astype(BF16)
        keep[0, k] = part[:rows]
        keep[1, k] = part[2 * rows : 3 * rows]
        d_copies.append(remote(dsnd.at[k], drcv.at[k], d_ss.at[k], d_rs.at[k], core_peer))
        d_copies[k].start()
        y_copies.append(remote(ysnd.at[k], yrcv.at[k], y_ss.at[k], y_rs.at[k], row_peer))
    for k in range(CHUNKS):
        d_copies[k].wait_recv()
        ysnd[k] = (keep[1, k] + drcv[k, 1].astype(F32)).astype(BF16)
        y_copies[k].start()
    for k in range(CHUNKS):
        y_copies[k].wait_recv()
        whole = keep[0, k] + drcv[k, 0].astype(F32) + yrcv[k].astype(F32)
        out_ref[:, k * step : (k + 1) * step] = whole.astype(BF16)
    for copy in pending + d_copies + y_copies:
        copy.wait_send()


def fused(tokens, w_query, w_key, w_value, w_out, mix_weight, out_gain):
    rows, width = tokens.shape
    nh = mix_weight.shape[0]
    vd = out_gain.shape[0]
    cols = w_query.shape[1]
    block = 4 * rows
    step = width // CHUNKS
    vmem, hbm = pl.BlockSpec(memory_space=pltpu.VMEM), pl.BlockSpec(memory_space=pl.ANY)
    dma = pltpu.SemaphoreType.DMA
    return pl.pallas_call(
        functools.partial(kernel, nh),
        out_shape=jax.ShapeDtypeStruct((rows, width), BF16),
        in_specs=[pl.BlockSpec(memory_space=pltpu.SMEM), vmem, vmem, hbm, hbm, hbm, hbm],
        out_specs=vmem,
        scratch_shapes=[
            pltpu.VMEM((width, cols), BF16),
            pltpu.VMEM((width, cols), BF16),
            pltpu.VMEM((width, cols), BF16),
            pltpu.VMEM(w_out.shape, BF16),
            pltpu.VMEM((3, rows, width), BF16),
            pltpu.VMEM((nh, 3, block, vd), BF16),
            pltpu.VMEM((3, nh * block, vd), BF16),
            pltpu.VMEM((2, nh * block, vd), BF16),
            pltpu.VMEM((nh - 1, block, vd), BF16),
            pltpu.VMEM((nh, block, vd), BF16),
            pltpu.VMEM((2, CHUNKS, rows, step), F32),
            pltpu.VMEM((CHUNKS, 2, rows, step), BF16),
            pltpu.VMEM((CHUNKS, 2, rows, step), BF16),
            pltpu.VMEM((CHUNKS, rows, step), BF16),
            pltpu.VMEM((CHUNKS, rows, step), BF16),
            dma((4,)), dma((3,)), dma((3,)),
            dma((2, nh - 1)), dma((2, nh - 1)), dma((2, nh)), dma((2, nh)),
            dma((nh - 1,)), dma((nh - 1,)),
            dma((CHUNKS,)), dma((CHUNKS,)), dma((CHUNKS,)), dma((CHUNKS,)),
        ],
        compiler_params=pltpu.CompilerParams(
            collective_id=0, has_side_effects=True, vmem_limit_bytes=56 * 2**20
        ),
    )(mix_weight, out_gain.reshape(1, vd), tokens, w_query, w_key, w_value, w_out)


def pick(mesh, *arrays):
    tokens, w_query, _, _, _, mix_weight, out_gain = arrays
    nh = mix_weight.shape[0]
    fits = (
        mesh.shape["sp"] == 2 * nh
        and mesh.shape["tp"] == 4
        and w_query.shape[1] == nh * out_gain.shape[0]
        and out_gain.shape[0] == 128
        and tokens.shape[0] % 16 == 0
        and tokens.shape[1] % (128 * CHUNKS) == 0
    )
    return fused(*arrays) if fits else shards(*arrays)


def solution(mesh):
    in_specs = (
        P(("sp", "tp"), None),
        P(None, "tp"),
        P(None, "tp"),
        P(None, "tp"),
        P("tp", None),
        P("tp"),
        P(),
    )
    out_specs = P(("sp", "tp"), None)
    return jax.shard_map(functools.partial(pick, mesh), mesh=mesh, in_specs=in_specs, out_specs=out_specs, check_vma=False)
```

```python
import functools
import math

import jax
import jax.numpy as jnp
from jax import lax
from jax.experimental import pallas as pl
from jax.experimental.pallas import tpu as pltpu
from jax.sharding import PartitionSpec as P


def block_rows(rows):
    best = 1
    for candidate in range(1, rows + 1):
        if rows % candidate == 0 and candidate <= 2048:
            best = candidate
    return best


def shards(tokens, w_query, w_key, w_value, w_out, mix_weight, out_gain):
    query_cols = w_query.shape[1]
    key_cols = w_key.shape[1]
    heads_here = mix_weight.shape[0]
    head_dim = query_cols // (2 * heads_here)
    value_dim = w_value.shape[1] // heads_here
    piece = lax.all_gather(tokens, "tp", axis=0, tiled=True)
    part_q = jnp.dot(piece, w_query, preferred_element_type=jnp.float32).astype(jnp.bfloat16)
    part_k = jnp.dot(piece, w_key, preferred_element_type=jnp.float32).astype(jnp.bfloat16)
    part_v = jnp.dot(piece, w_value, preferred_element_type=jnp.float32).astype(jnp.bfloat16)
    joined = jnp.concatenate([part_q, part_k, part_v], axis=1)
    queries = joined[:, :query_cols]
    keys = joined[:, query_cols : query_cols + key_cols]
    values = joined[:, query_cols + key_cols :]
    n_query = queries.shape[0]
    query_four = queries.reshape(n_query, heads_here, 2, head_dim)
    scale = head_dim ** (-0.5)

    def step(carry, block):
        running_max, running_sum, accum = carry
        key_blk, value_blk = block
        scores = (
            jnp.einsum("qhmd,khmd->hmqk", query_four, key_blk, preferred_element_type=jnp.float32)
            * scale
        )
        new_max = jnp.maximum(running_max, jnp.max(scores, axis=-1))
        factor = jnp.exp(running_max - new_max)
        expw = jnp.exp(scores - new_max[..., None])
        running_sum = running_sum * factor + jnp.sum(expw, axis=-1)
        weights = expw.astype(jnp.bfloat16)
        accum = accum * factor[..., None] + jnp.einsum(
            "hmqk,khe->hmqe", weights, value_blk, preferred_element_type=jnp.float32
        )
        return ((new_max, running_sum, accum), None)

    initial = (
        jnp.full((heads_here, 2, n_query), -1e30, jnp.float32),
        jnp.zeros((heads_here, 2, n_query), jnp.float32),
        jnp.zeros((heads_here, 2, n_query, value_dim), jnp.float32),
    )
    all_keys, all_values = (
        lax.all_gather(keys, "sp", axis=0, tiled=True),
        lax.all_gather(values, "sp", axis=0, tiled=True),
    )
    carry = initial
    rows = all_keys.shape[0]
    group = block_rows(rows)
    key_blocks = all_keys.reshape(rows // group, group, heads_here, 2, head_dim)
    value_blocks = all_values.reshape(rows // group, group, heads_here, value_dim)
    carry, unused = lax.scan(step, carry, (key_blocks, value_blocks))
    running_max, running_sum, accum = carry
    heads_out = (
        accum[:, 0] / running_sum[:, 0, :, None]
        - mix_weight[:, None, None] * accum[:, 1] / running_sum[:, 1, :, None]
    )
    meansq = jnp.mean(heads_out * heads_out, axis=-1, keepdims=True)
    normed = (heads_out * lax.rsqrt(meansq + 1e-06) * out_gain).astype(jnp.bfloat16)
    normed = normed.transpose(1, 0, 2).reshape(n_query, heads_here * value_dim)
    return lax.psum_scatter(
        jnp.dot(normed, w_out, preferred_element_type=jnp.float32).astype(jnp.bfloat16),
        "tp",
        scatter_dimension=0,
        tiled=True,
    )


BF16 = jnp.bfloat16
F32 = jnp.float32
MESH = pl.DeviceIdType.MESH
CHUNKS = 4


def remote(src, dst, send, recv, where):
    return pltpu.make_async_remote_copy(
        src_ref=src, dst_ref=dst, send_sem=send, recv_sem=recv, device_id=where, device_id_type=MESH
    )


def kernel(
    nh, mix_ref, gain_ref, tok_ref, wq_hbm, wk_hbm, wv_hbm, wo_hbm, out_ref,
    wq, wk, wv, wo, tok, snd, rcv, kvx, nsnd, nrm, keep, dsnd, drcv, ysnd, yrcv,
    w_sem, a_ss, a_rs, z_ss, z_rs, x_ss, x_rs, c_ss, c_rs, d_ss, d_rs, y_ss, y_rs,
):
    rows, width = tok_ref.shape
    pair = 2 * rows
    vd = gain_ref.shape[1]
    s, t = lax.axis_index("sp"), lax.axis_index("tp")
    h, g = s // 2, s % 2
    core_peer = {"tp": t + 1 - 2 * (t % 2)}
    row_peer = {"tp": t + 2 - 4 * (t // 2)}
    side_peer = {"sp": h * 2 + (1 - g)}

    def head_peer(d):
        return {"sp": lax.rem(h + d, nh) * 2 + g}

    loads = [
        pltpu.make_async_copy(a, b, w_sem.at[i])
        for i, (a, b) in enumerate(((wq_hbm, wq), (wk_hbm, wk), (wv_hbm, wv), (wo_hbm, wo)))
    ]
    for load in loads:
        load.start()

    barrier = pltpu.get_barrier_semaphore()
    peers = [core_peer, row_peer, side_peer] + [head_peer(d) for d in range(1, nh)]
    for peer in peers:
        pl.semaphore_signal(barrier, inc=1, device_id=peer, device_id_type=MESH)
    pl.semaphore_wait(barrier, len(peers))

    pending = []
    to_row = remote(tok_ref, tok.at[1], a_ss.at[1], a_rs.at[1], row_peer)
    to_row.start()
    to_core = remote(tok_ref, tok.at[0], a_ss.at[0], a_rs.at[0], core_peer)
    to_core.start()
    forward = remote(tok.at[1], tok.at[2], a_ss.at[2], a_rs.at[2], core_peer)
    pending += [to_row, to_core, forward]

    half = nh * pair
    z_copies, q_copies, x_copies = {}, {}, {}

    def at(p, d):
        return pl.ds(p * half + d * pair, pair)

    def project(p, x):
        mine = pl.ds(p * pair, pair)
        for i, w in enumerate((wq, wk, wv)):
            if p == 0:
                loads[i].wait()
            y = jnp.dot(x, w[...], preferred_element_type=F32).astype(BF16)
            for hh in range(nh):
                snd[hh, i, mine, :] = y[:, hh * vd : (hh + 1) * vd]
        x_copies[p, 0] = remote(
            snd.at[h, pl.ds(1, 2), mine, :], kvx.at[:, at(p, 0), :], x_ss.at[p, 0], x_rs.at[p, 0], side_peer
        )
        x_copies[p, 0].start()
        for copies, i, n, sem in ((z_copies, 1, 2, 0), (q_copies, 0, 1, 1)):
            for d in range(1, nh):
                copies[p, d] = remote(
                    snd.at[lax.rem(h + d, nh), pl.ds(i, n), mine, :],
                    rcv.at[pl.ds(i, n), at(p, d), :],
                    z_ss.at[sem, p, d - 1],
                    z_rs.at[sem, p, d - 1],
                    head_peer(d),
                )
                copies[p, d].start()
        rcv[:, at(p, 0), :] = snd[h, :, mine, :]

    def relay(p):
        for d in range(1, nh):
            z_copies[p, d].wait_recv()
            x_copies[p, d] = remote(
                rcv.at[pl.ds(1, 2), at(p, d), :], kvx.at[:, at(p, d), :], x_ss.at[p, d], x_rs.at[p, d], side_peer
            )
            x_copies[p, d].start()

    hd = vd // 2
    c = (hd ** -0.5) * math.log2(math.e)
    lam = mix_ref[h]
    gain = gain_ref[...]
    lane = lax.broadcasted_iota(jnp.int32, (half, vd), 1)
    nt = (((1,), (1,)), ((), ()))
    state = {}

    def attend(p, k, v):
        q = rcv[0, pl.ds(p * half, half), :]
        zero = jnp.zeros_like(q)
        qq = jnp.concatenate([jnp.where(lane < hd, q, zero), jnp.where(lane < hd, zero, q)], axis=0)
        scores = lax.dot_general(qq, k, nt, preferred_element_type=F32)
        top = jnp.max(scores, axis=1, keepdims=True)
        if p in state:
            top = jnp.maximum(top, state[p][0])
        expw = jnp.exp2((scores - top) * c)
        total = jnp.sum(expw, axis=1, keepdims=True)
        acc = jnp.dot(expw.astype(BF16), v, preferred_element_type=F32)
        if p in state:
            factor = jnp.exp2((state[p][0] - top) * c)
            total = total + state[p][1] * factor
            acc = acc + state[p][2] * factor
        state[p] = (top, total, acc)

    def own(p, kp):
        attend(p, rcv[1, pl.ds(kp * half, half), :], rcv[2, pl.ds(kp * half, half), :])

    def side(p, kp):
        attend(p, kvx[0, pl.ds(kp * half, half), :], kvx[1, pl.ds(kp * half, half), :])

    c_copies = {}

    def finish(p):
        _, total, acc = state[p]
        o = acc / total
        o = o[:half] - lam * o[half:]
        meansq = jnp.mean(o * o, axis=1, keepdims=True)
        normed = (o * lax.rsqrt(meansq + 1e-06) * gain).astype(BF16)
        for d in range(1, nh):
            nsnd[p, d - 1] = normed[d * pair : (d + 1) * pair]
            c_copies[p, d] = remote(
                nsnd.at[p, d - 1], nrm.at[p, h], c_ss.at[p, d - 1], c_rs.at[p, d - 1], head_peer(nh - d)
            )
            c_copies[p, d].start()
        nrm[p, h] = normed[:pair]

    def arrived(copies, p):
        for (cp, d), copy in copies.items():
            if cp == p:
                copy.wait_recv()

    to_core.wait_recv()
    project(0, jnp.concatenate([tok_ref[...], tok[0]], axis=0))
    to_row.wait_recv()
    forward.start()
    forward.wait_recv()
    project(1, tok[1:3].reshape(pair, width))
    relay(0)
    arrived(q_copies, 0)
    own(0, 0)
    arrived(x_copies, 0)
    side(0, 0)
    relay(1)
    own(0, 1)
    arrived(q_copies, 1)
    own(1, 0)
    side(1, 0)
    own(1, 1)
    arrived(x_copies, 1)
    side(1, 1)
    finish(1)
    side(0, 1)
    finish(0)

    step = width // CHUNKS
    d_copies, y_copies = {}, []

    def out_part(p):
        arrived(c_copies, p)
        n = jnp.concatenate([nrm[p, i] for i in range(nh)], axis=1)
        for k in range(CHUNKS):
            part = jnp.dot(n, wo[:, k * step : (k + 1) * step], preferred_element_type=F32)
            dsnd[p, k] = part[rows:].astype(BF16)
            keep[p, k] = part[:rows]
            d_copies[p, k] = remote(dsnd.at[p, k], drcv.at[p, k], d_ss.at[p, k], d_rs.at[p, k], core_peer)
            d_copies[p, k].start()

    loads[3].wait()
    out_part(1)
    for k in range(CHUNKS):
        d_copies[1, k].wait_recv()
        ysnd[k] = (keep[1, k] + drcv[1, k].astype(F32)).astype(BF16)
        y_copies.append(remote(ysnd.at[k], yrcv.at[k], y_ss.at[k], y_rs.at[k], row_peer))
        y_copies[k].start()
    out_part(0)
    for k in range(CHUNKS):
        d_copies[0, k].wait_recv()
        y_copies[k].wait_recv()
        whole = keep[0, k] + drcv[0, k].astype(F32) + yrcv[k].astype(F32)
        out_ref[:, k * step : (k + 1) * step] = whole.astype(BF16)
    for copies in (z_copies, q_copies, x_copies, c_copies, d_copies):
        pending += list(copies.values())
    for copy in pending + y_copies:
        copy.wait_send()


def fused(tokens, w_query, w_key, w_value, w_out, mix_weight, out_gain):
    rows, width = tokens.shape
    nh = mix_weight.shape[0]
    vd = out_gain.shape[0]
    cols = w_query.shape[1]
    block = 4 * rows
    step = width // CHUNKS
    vmem, hbm = pl.BlockSpec(memory_space=pltpu.VMEM), pl.BlockSpec(memory_space=pl.ANY)
    dma = pltpu.SemaphoreType.DMA
    return pl.pallas_call(
        functools.partial(kernel, nh),
        out_shape=jax.ShapeDtypeStruct((rows, width), BF16),
        in_specs=[pl.BlockSpec(memory_space=pltpu.SMEM), vmem, vmem, hbm, hbm, hbm, hbm],
        out_specs=vmem,
        scratch_shapes=[
            pltpu.VMEM((width, cols), BF16),
            pltpu.VMEM((width, cols), BF16),
            pltpu.VMEM((width, cols), BF16),
            pltpu.VMEM(w_out.shape, BF16),
            pltpu.VMEM((3, rows, width), BF16),
            pltpu.VMEM((nh, 3, block, vd), BF16),
            pltpu.VMEM((3, nh * block, vd), BF16),
            pltpu.VMEM((2, nh * block, vd), BF16),
            pltpu.VMEM((2, nh - 1, 2 * rows, vd), BF16),
            pltpu.VMEM((2, nh, 2 * rows, vd), BF16),
            pltpu.VMEM((2, CHUNKS, rows, step), F32),
            pltpu.VMEM((2, CHUNKS, rows, step), BF16),
            pltpu.VMEM((2, CHUNKS, rows, step), BF16),
            pltpu.VMEM((CHUNKS, rows, step), BF16),
            pltpu.VMEM((CHUNKS, rows, step), BF16),
            dma((4,)), dma((3,)), dma((3,)),
            dma((2, 2, nh - 1)), dma((2, 2, nh - 1)), dma((2, nh)), dma((2, nh)),
            dma((2, nh - 1)), dma((2, nh - 1)),
            dma((2, CHUNKS)), dma((2, CHUNKS)), dma((CHUNKS,)), dma((CHUNKS,)),
        ],
        compiler_params=pltpu.CompilerParams(
            collective_id=0, has_side_effects=True, vmem_limit_bytes=56 * 2**20
        ),
    )(mix_weight, out_gain.reshape(1, vd), tokens, w_query, w_key, w_value, w_out)


def pick(mesh, *arrays):
    tokens, w_query, _, _, _, mix_weight, out_gain = arrays
    nh = mix_weight.shape[0]
    fits = (
        mesh.shape["sp"] == 2 * nh
        and mesh.shape["tp"] == 4
        and w_query.shape[1] == nh * out_gain.shape[0]
        and out_gain.shape[0] == 128
        and tokens.shape[0] % 16 == 0
        and tokens.shape[1] % (128 * CHUNKS) == 0
    )
    return fused(*arrays) if fits else shards(*arrays)


def solution(mesh):
    in_specs = (
        P(("sp", "tp"), None),
        P(None, "tp"),
        P(None, "tp"),
        P(None, "tp"),
        P("tp", None),
        P("tp"),
        P(),
    )
    out_specs = P(("sp", "tp"), None)
    return jax.shard_map(functools.partial(pick, mesh), mesh=mesh, in_specs=in_specs, out_specs=out_specs, check_vma=False)
```

```python
import functools
import math

import jax
import jax.numpy as jnp
from jax import lax
from jax.experimental import pallas as pl
from jax.experimental.pallas import tpu as pltpu
from jax.sharding import PartitionSpec as P


def block_rows(rows):
    best = 1
    for candidate in range(1, rows + 1):
        if rows % candidate == 0 and candidate <= 2048:
            best = candidate
    return best


def shards(tokens, w_query, w_key, w_value, w_out, mix_weight, out_gain):
    query_cols = w_query.shape[1]
    key_cols = w_key.shape[1]
    heads_here = mix_weight.shape[0]
    head_dim = query_cols // (2 * heads_here)
    value_dim = w_value.shape[1] // heads_here
    piece = lax.all_gather(tokens, "tp", axis=0, tiled=True)
    part_q = jnp.dot(piece, w_query, preferred_element_type=jnp.float32).astype(jnp.bfloat16)
    part_k = jnp.dot(piece, w_key, preferred_element_type=jnp.float32).astype(jnp.bfloat16)
    part_v = jnp.dot(piece, w_value, preferred_element_type=jnp.float32).astype(jnp.bfloat16)
    joined = jnp.concatenate([part_q, part_k, part_v], axis=1)
    queries = joined[:, :query_cols]
    keys = joined[:, query_cols : query_cols + key_cols]
    values = joined[:, query_cols + key_cols :]
    n_query = queries.shape[0]
    query_four = queries.reshape(n_query, heads_here, 2, head_dim)
    scale = head_dim ** (-0.5)

    def step(carry, block):
        running_max, running_sum, accum = carry
        key_blk, value_blk = block
        scores = (
            jnp.einsum("qhmd,khmd->hmqk", query_four, key_blk, preferred_element_type=jnp.float32)
            * scale
        )
        new_max = jnp.maximum(running_max, jnp.max(scores, axis=-1))
        factor = jnp.exp(running_max - new_max)
        expw = jnp.exp(scores - new_max[..., None])
        running_sum = running_sum * factor + jnp.sum(expw, axis=-1)
        weights = expw.astype(jnp.bfloat16)
        accum = accum * factor[..., None] + jnp.einsum(
            "hmqk,khe->hmqe", weights, value_blk, preferred_element_type=jnp.float32
        )
        return ((new_max, running_sum, accum), None)

    initial = (
        jnp.full((heads_here, 2, n_query), -1e30, jnp.float32),
        jnp.zeros((heads_here, 2, n_query), jnp.float32),
        jnp.zeros((heads_here, 2, n_query, value_dim), jnp.float32),
    )
    all_keys, all_values = (
        lax.all_gather(keys, "sp", axis=0, tiled=True),
        lax.all_gather(values, "sp", axis=0, tiled=True),
    )
    carry = initial
    rows = all_keys.shape[0]
    group = block_rows(rows)
    key_blocks = all_keys.reshape(rows // group, group, heads_here, 2, head_dim)
    value_blocks = all_values.reshape(rows // group, group, heads_here, value_dim)
    carry, unused = lax.scan(step, carry, (key_blocks, value_blocks))
    running_max, running_sum, accum = carry
    heads_out = (
        accum[:, 0] / running_sum[:, 0, :, None]
        - mix_weight[:, None, None] * accum[:, 1] / running_sum[:, 1, :, None]
    )
    meansq = jnp.mean(heads_out * heads_out, axis=-1, keepdims=True)
    normed = (heads_out * lax.rsqrt(meansq + 1e-06) * out_gain).astype(jnp.bfloat16)
    normed = normed.transpose(1, 0, 2).reshape(n_query, heads_here * value_dim)
    return lax.psum_scatter(
        jnp.dot(normed, w_out, preferred_element_type=jnp.float32).astype(jnp.bfloat16),
        "tp",
        scatter_dimension=0,
        tiled=True,
    )


BF16 = jnp.bfloat16
F32 = jnp.float32
MESH = pl.DeviceIdType.MESH
CHUNKS = 4


def remote(src, dst, send, recv, where):
    return pltpu.make_async_remote_copy(
        src_ref=src, dst_ref=dst, send_sem=send, recv_sem=recv, device_id=where, device_id_type=MESH
    )


def kernel(
    nh, mix_ref, gain_ref, tok_ref, wq_hbm, wk_hbm, wv_hbm, wo_hbm, out_ref,
    wq, wk, wv, wo, tok, snd, rcv, kvx, nsnd, nrm, keep, dsnd, drcv, ysnd, yrcv,
    w_sem, a_ss, a_rs, z_ss, z_rs, x_ss, x_rs, c_ss, c_rs, d_ss, d_rs, y_ss, y_rs,
):
    rows, width = tok_ref.shape
    pair = 2 * rows
    vd = gain_ref.shape[1]
    s, t = lax.axis_index("sp"), lax.axis_index("tp")
    h, g = s // 2, s % 2
    core_peer = {"tp": t + 1 - 2 * (t % 2)}
    row_peer = {"tp": t + 2 - 4 * (t // 2)}
    side_peer = {"sp": h * 2 + (1 - g)}

    def head_peer(d):
        return {"sp": lax.rem(h + d, nh) * 2 + g}

    loads = [
        pltpu.make_async_copy(a, b, w_sem.at[i])
        for i, (a, b) in enumerate(((wq_hbm, wq), (wk_hbm, wk), (wv_hbm, wv), (wo_hbm, wo)))
    ]
    for load in loads:
        load.start()

    barrier = pltpu.get_barrier_semaphore()
    peers = [core_peer, row_peer, side_peer] + [head_peer(d) for d in range(1, nh)]
    for peer in peers:
        pl.semaphore_signal(barrier, inc=1, device_id=peer, device_id_type=MESH)

    pending = []
    half = nh * pair
    z_copies, q_copies, x_copies = {}, {}, {}

    quarter = nh * rows

    def at(u, d):
        return pl.ds(u * quarter + d * rows, rows)

    def project(u, x):
        for i, w in ((1, wk), (2, wv), (0, wq)):
            if u == 0:
                loads[i].wait()
            y = jnp.dot(x, w[...], preferred_element_type=F32).astype(BF16)
            for hh in range(nh):
                snd[hh, i, pl.ds(u * rows, rows), :] = y[:, hh * vd : (hh + 1) * vd]
        rcv[:, at(u, 0), :] = snd[h, :, pl.ds(u * rows, rows), :]

    def send(u):
        mine = pl.ds(u * rows, rows)
        for copies, i, n, sem in ((z_copies, 1, 2, 0), (q_copies, 0, 1, 1)):
            for d in range(1, nh):
                copies[u, d] = remote(
                    snd.at[lax.rem(h + d, nh), pl.ds(i, n), mine, :],
                    rcv.at[pl.ds(i, n), at(u, d), :],
                    z_ss.at[sem, u, d - 1],
                    z_rs.at[sem, u, d - 1],
                    head_peer(d),
                )
                copies[u, d].start()
        x_copies[u, 0] = remote(
            snd.at[h, pl.ds(1, 2), mine, :], kvx.at[:, at(u, 0), :], x_ss.at[u, 0], x_rs.at[u, 0], side_peer
        )
        x_copies[u, 0].start()

    def relay(u):
        for d in range(1, nh):
            z_copies[u, d].wait_recv()
            x_copies[u, d] = remote(
                rcv.at[pl.ds(1, 2), at(u, d), :], kvx.at[:, at(u, d), :], x_ss.at[u, d], x_rs.at[u, d], side_peer
            )
            x_copies[u, d].start()

    hd = vd // 2
    c = (hd ** -0.5) * math.log2(math.e)
    lam = mix_ref[h]
    gain = gain_ref[...]
    lane = lax.broadcasted_iota(jnp.int32, (half, vd), 1)
    nt = (((1,), (1,)), ((), ()))
    state = {}

    def attend(p, k, v):
        q = rcv[0, pl.ds(p * half, half), :]
        zero = jnp.zeros_like(q)
        qq = jnp.concatenate([jnp.where(lane < hd, q, zero), jnp.where(lane < hd, zero, q)], axis=0)
        scores = lax.dot_general(qq, k, nt, preferred_element_type=F32)
        top = jnp.max(scores, axis=1, keepdims=True)
        if p in state:
            top = jnp.maximum(top, state[p][0])
        expw = jnp.exp2((scores - top) * c)
        total = jnp.sum(expw, axis=1, keepdims=True)
        acc = jnp.dot(expw.astype(BF16), v, preferred_element_type=F32)
        if p in state:
            factor = jnp.exp2((state[p][0] - top) * c)
            total = total + state[p][1] * factor
            acc = acc + state[p][2] * factor
        state[p] = (top, total, acc)

    def own(p, kp):
        attend(p, rcv[1, pl.ds(kp * half, half), :], rcv[2, pl.ds(kp * half, half), :])

    def side(p, kp):
        attend(p, kvx[0, pl.ds(kp * half, half), :], kvx[1, pl.ds(kp * half, half), :])

    c_copies = {}

    def finish(p):
        _, total, acc = state[p]
        o = acc / total
        o = o[:half] - lam * o[half:]
        meansq = jnp.mean(o * o, axis=1, keepdims=True)
        normed = (o * lax.rsqrt(meansq + 1e-06) * gain).astype(BF16)
        normed = normed.reshape(2, nh, rows, vd)
        for d in range(1, nh):
            nsnd[p, d - 1] = normed[:, d]
            c_copies[p, d] = remote(
                nsnd.at[p, d - 1], nrm.at[p, h], c_ss.at[p, d - 1], c_rs.at[p, d - 1], head_peer(nh - d)
            )
            c_copies[p, d].start()
        nrm[p, h] = normed[:, 0]

    def arrived(copies, p):
        for (cp, d), copy in copies.items():
            if cp == p:
                copy.wait_recv()

    project(0, tok_ref[...])
    pl.semaphore_wait(barrier, len(peers))
    to_row = remote(tok_ref, tok.at[1], a_ss.at[1], a_rs.at[1], row_peer)
    to_row.start()
    to_core = remote(tok_ref, tok.at[0], a_ss.at[0], a_rs.at[0], core_peer)
    to_core.start()
    forward = remote(tok.at[1], tok.at[2], a_ss.at[2], a_rs.at[2], core_peer)
    pending += [to_row, to_core, forward]
    send(0)
    to_core.wait_recv()
    project(1, tok[0])
    send(1)
    to_row.wait_recv()
    forward.start()
    project(2, tok[1])
    send(2)
    forward.wait_recv()
    project(3, tok[2])
    send(3)
    relay(0)
    relay(1)
    for u in range(2):
        arrived(q_copies, u)
    own(0, 0)
    relay(2)
    for u in range(2):
        arrived(x_copies, u)
    side(0, 0)
    relay(3)
    own(0, 1)
    for u in range(2, 4):
        arrived(q_copies, u)
    own(1, 0)
    side(1, 0)
    own(1, 1)
    for u in range(2, 4):
        arrived(x_copies, u)
    side(1, 1)
    finish(1)
    side(0, 1)
    finish(0)

    step = width // CHUNKS
    d_copies, y_copies = {}, []

    def out_part(p):
        arrived(c_copies, p)
        n = jnp.concatenate([nrm[p, i].reshape(pair, vd) for i in range(nh)], axis=1)
        for k in range(CHUNKS):
            part = jnp.dot(n, wo[:, k * step : (k + 1) * step], preferred_element_type=F32)
            dsnd[p, k] = part[rows:].astype(BF16)
            keep[p, k] = part[:rows]
            d_copies[p, k] = remote(dsnd.at[p, k], drcv.at[p, k], d_ss.at[p, k], d_rs.at[p, k], core_peer)
            d_copies[p, k].start()

    loads[3].wait()
    out_part(1)
    for k in range(CHUNKS):
        d_copies[1, k].wait_recv()
        ysnd[k] = (keep[1, k] + drcv[1, k].astype(F32)).astype(BF16)
        y_copies.append(remote(ysnd.at[k], yrcv.at[k], y_ss.at[k], y_rs.at[k], row_peer))
        y_copies[k].start()
    out_part(0)
    for k in range(CHUNKS):
        d_copies[0, k].wait_recv()
        y_copies[k].wait_recv()
        whole = keep[0, k] + drcv[0, k].astype(F32) + yrcv[k].astype(F32)
        out_ref[:, k * step : (k + 1) * step] = whole.astype(BF16)
    for copies in (z_copies, q_copies, x_copies, c_copies, d_copies):
        pending += list(copies.values())
    for copy in pending + y_copies:
        copy.wait_send()


def fused(tokens, w_query, w_key, w_value, w_out, mix_weight, out_gain):
    rows, width = tokens.shape
    nh = mix_weight.shape[0]
    vd = out_gain.shape[0]
    cols = w_query.shape[1]
    block = 4 * rows
    step = width // CHUNKS
    vmem, hbm = pl.BlockSpec(memory_space=pltpu.VMEM), pl.BlockSpec(memory_space=pl.ANY)
    dma = pltpu.SemaphoreType.DMA
    return pl.pallas_call(
        functools.partial(kernel, nh),
        out_shape=jax.ShapeDtypeStruct((rows, width), BF16),
        in_specs=[pl.BlockSpec(memory_space=pltpu.SMEM), vmem, vmem, hbm, hbm, hbm, hbm],
        out_specs=vmem,
        scratch_shapes=[
            pltpu.VMEM((width, cols), BF16),
            pltpu.VMEM((width, cols), BF16),
            pltpu.VMEM((width, cols), BF16),
            pltpu.VMEM(w_out.shape, BF16),
            pltpu.VMEM((3, rows, width), BF16),
            pltpu.VMEM((nh, 3, block, vd), BF16),
            pltpu.VMEM((3, nh * block, vd), BF16),
            pltpu.VMEM((2, nh * block, vd), BF16),
            pltpu.VMEM((2, nh - 1, 2, rows, vd), BF16),
            pltpu.VMEM((2, nh, 2, rows, vd), BF16),
            pltpu.VMEM((2, CHUNKS, rows, step), F32),
            pltpu.VMEM((2, CHUNKS, rows, step), BF16),
            pltpu.VMEM((2, CHUNKS, rows, step), BF16),
            pltpu.VMEM((CHUNKS, rows, step), BF16),
            pltpu.VMEM((CHUNKS, rows, step), BF16),
            dma((4,)), dma((3,)), dma((3,)),
            dma((2, 4, nh - 1)), dma((2, 4, nh - 1)), dma((4, nh)), dma((4, nh)),
            dma((2, nh - 1)), dma((2, nh - 1)),
            dma((2, CHUNKS)), dma((2, CHUNKS)), dma((CHUNKS,)), dma((CHUNKS,)),
        ],
        compiler_params=pltpu.CompilerParams(
            collective_id=0, has_side_effects=True, vmem_limit_bytes=56 * 2**20
        ),
    )(mix_weight, out_gain.reshape(1, vd), tokens, w_query, w_key, w_value, w_out)


def pick(mesh, *arrays):
    tokens, w_query, _, _, _, mix_weight, out_gain = arrays
    nh = mix_weight.shape[0]
    fits = (
        mesh.shape["sp"] == 2 * nh
        and mesh.shape["tp"] == 4
        and w_query.shape[1] == nh * out_gain.shape[0]
        and out_gain.shape[0] == 128
        and tokens.shape[0] % 16 == 0
        and tokens.shape[1] % (128 * CHUNKS) == 0
    )
    return fused(*arrays) if fits else shards(*arrays)


def solution(mesh):
    in_specs = (
        P(("sp", "tp"), None),
        P(None, "tp"),
        P(None, "tp"),
        P(None, "tp"),
        P("tp", None),
        P("tp"),
        P(),
    )
    out_specs = P(("sp", "tp"), None)
    return jax.shard_map(functools.partial(pick, mesh), mesh=mesh, in_specs=in_specs, out_specs=out_specs, check_vma=False)
```

```python
import functools
import math

import jax
import jax.numpy as jnp
from jax import lax
from jax.experimental import pallas as pl
from jax.experimental.pallas import tpu as pltpu
from jax.sharding import PartitionSpec as P


def block_rows(rows):
    best = 1
    for candidate in range(1, rows + 1):
        if rows % candidate == 0 and candidate <= 2048:
            best = candidate
    return best


def shards(tokens, w_query, w_key, w_value, w_out, mix_weight, out_gain):
    query_cols = w_query.shape[1]
    key_cols = w_key.shape[1]
    heads_here = mix_weight.shape[0]
    head_dim = query_cols // (2 * heads_here)
    value_dim = w_value.shape[1] // heads_here
    piece = lax.all_gather(tokens, "tp", axis=0, tiled=True)
    part_q = jnp.dot(piece, w_query, preferred_element_type=jnp.float32).astype(jnp.bfloat16)
    part_k = jnp.dot(piece, w_key, preferred_element_type=jnp.float32).astype(jnp.bfloat16)
    part_v = jnp.dot(piece, w_value, preferred_element_type=jnp.float32).astype(jnp.bfloat16)
    joined = jnp.concatenate([part_q, part_k, part_v], axis=1)
    queries = joined[:, :query_cols]
    keys = joined[:, query_cols : query_cols + key_cols]
    values = joined[:, query_cols + key_cols :]
    n_query = queries.shape[0]
    query_four = queries.reshape(n_query, heads_here, 2, head_dim)
    scale = head_dim ** (-0.5)

    def step(carry, block):
        running_max, running_sum, accum = carry
        key_blk, value_blk = block
        scores = (
            jnp.einsum("qhmd,khmd->hmqk", query_four, key_blk, preferred_element_type=jnp.float32)
            * scale
        )
        new_max = jnp.maximum(running_max, jnp.max(scores, axis=-1))
        factor = jnp.exp(running_max - new_max)
        expw = jnp.exp(scores - new_max[..., None])
        running_sum = running_sum * factor + jnp.sum(expw, axis=-1)
        weights = expw.astype(jnp.bfloat16)
        accum = accum * factor[..., None] + jnp.einsum(
            "hmqk,khe->hmqe", weights, value_blk, preferred_element_type=jnp.float32
        )
        return ((new_max, running_sum, accum), None)

    initial = (
        jnp.full((heads_here, 2, n_query), -1e30, jnp.float32),
        jnp.zeros((heads_here, 2, n_query), jnp.float32),
        jnp.zeros((heads_here, 2, n_query, value_dim), jnp.float32),
    )
    all_keys, all_values = (
        lax.all_gather(keys, "sp", axis=0, tiled=True),
        lax.all_gather(values, "sp", axis=0, tiled=True),
    )
    carry = initial
    rows = all_keys.shape[0]
    group = block_rows(rows)
    key_blocks = all_keys.reshape(rows // group, group, heads_here, 2, head_dim)
    value_blocks = all_values.reshape(rows // group, group, heads_here, value_dim)
    carry, unused = lax.scan(step, carry, (key_blocks, value_blocks))
    running_max, running_sum, accum = carry
    heads_out = (
        accum[:, 0] / running_sum[:, 0, :, None]
        - mix_weight[:, None, None] * accum[:, 1] / running_sum[:, 1, :, None]
    )
    meansq = jnp.mean(heads_out * heads_out, axis=-1, keepdims=True)
    normed = (heads_out * lax.rsqrt(meansq + 1e-06) * out_gain).astype(jnp.bfloat16)
    normed = normed.transpose(1, 0, 2).reshape(n_query, heads_here * value_dim)
    return lax.psum_scatter(
        jnp.dot(normed, w_out, preferred_element_type=jnp.float32).astype(jnp.bfloat16),
        "tp",
        scatter_dimension=0,
        tiled=True,
    )


BF16 = jnp.bfloat16
F32 = jnp.float32
MESH = pl.DeviceIdType.MESH
CHUNKS = 4


def remote(src, dst, send, recv, where):
    return pltpu.make_async_remote_copy(
        src_ref=src, dst_ref=dst, send_sem=send, recv_sem=recv, device_id=where, device_id_type=MESH
    )


def kernel(
    nh, mix_ref, gain_ref, tok_ref, wq_hbm, wk_hbm, wv_hbm, wo_hbm, out_ref,
    wq, wk, wv, wo, tok, snd, rcv, kvx, nsnd, nrm, keep, dsnd, drcv, ysnd, yrcv,
    w_sem, a_ss, a_rs, z_ss, z_rs, x_ss, x_rs, c_ss, c_rs, d_ss, d_rs, y_ss, y_rs,
):
    rows, width = tok_ref.shape
    pair = 2 * rows
    vd = gain_ref.shape[1]
    s, t = lax.axis_index("sp"), lax.axis_index("tp")
    h, g = s // 2, s % 2
    core_peer = {"tp": t + 1 - 2 * (t % 2)}
    row_peer = {"tp": t + 2 - 4 * (t // 2)}
    side_peer = {"sp": h * 2 + (1 - g)}

    def head_peer(d):
        return {"sp": lax.rem(h + d, nh) * 2 + g}

    loads = [
        pltpu.make_async_copy(a, b, w_sem.at[i])
        for i, (a, b) in enumerate(((wq_hbm, wq), (wk_hbm, wk), (wv_hbm, wv), (wo_hbm, wo)))
    ]
    for load in loads:
        load.start()

    barrier = pltpu.get_barrier_semaphore()
    peers = [core_peer, row_peer, side_peer] + [head_peer(d) for d in range(1, nh)]
    for peer in peers:
        pl.semaphore_signal(barrier, inc=1, device_id=peer, device_id_type=MESH)

    pending = []
    half = nh * pair
    z_copies, q_copies, x_copies = {}, {}, {}

    quarter = nh * rows

    def at(u, d):
        return pl.ds(u * quarter + d * rows, rows)

    def project(u, x):
        for i, w in ((1, wk), (2, wv), (0, wq)):
            if u == 0:
                loads[i].wait()
            y = jnp.dot(x, w[...], preferred_element_type=F32).astype(BF16)
            for hh in range(nh):
                snd[hh, i, pl.ds(u * rows, rows), :] = y[:, hh * vd : (hh + 1) * vd]
        rcv[:, at(u, 0), :] = snd[h, :, pl.ds(u * rows, rows), :]

    def spread(copies, u, i, n, sem):
        for d in range(1, nh):
            copies[u, d] = remote(
                snd.at[lax.rem(h + d, nh), pl.ds(i, n), pl.ds(u * rows, rows), :],
                rcv.at[pl.ds(i, n), at(u, d), :],
                z_ss.at[sem, u, d - 1],
                z_rs.at[sem, u, d - 1],
                head_peer(d),
            )
            copies[u, d].start()

    def send_q(u):
        spread(q_copies, u, 0, 1, 1)

    def send_kv(u):
        spread(z_copies, u, 1, 2, 0)
        x_copies[u, 0] = remote(
            snd.at[h, pl.ds(1, 2), pl.ds(u * rows, rows), :],
            kvx.at[:, at(u, 0), :],
            x_ss.at[u, 0],
            x_rs.at[u, 0],
            side_peer,
        )
        x_copies[u, 0].start()

    def relay(u):
        for d in range(1, nh):
            z_copies[u, d].wait_recv()
            x_copies[u, d] = remote(
                rcv.at[pl.ds(1, 2), at(u, d), :], kvx.at[:, at(u, d), :], x_ss.at[u, d], x_rs.at[u, d], side_peer
            )
            x_copies[u, d].start()

    hd = vd // 2
    c = (hd ** -0.5) * math.log2(math.e)
    lam = mix_ref[h]
    gain = gain_ref[...]
    lane = lax.broadcasted_iota(jnp.int32, (half, vd), 1)
    nt = (((1,), (1,)), ((), ()))
    state = {}

    def attend(p, k, v):
        q = rcv[0, pl.ds(p * half, half), :]
        zero = jnp.zeros_like(q)
        qq = jnp.concatenate([jnp.where(lane < hd, q, zero), jnp.where(lane < hd, zero, q)], axis=0)
        scores = lax.dot_general(qq, k, nt, preferred_element_type=F32)
        top = jnp.max(scores, axis=1, keepdims=True)
        if p in state:
            top = jnp.maximum(top, state[p][0])
        expw = jnp.exp2((scores - top) * c)
        total = jnp.sum(expw, axis=1, keepdims=True)
        acc = jnp.dot(expw.astype(BF16), v, preferred_element_type=F32)
        if p in state:
            factor = jnp.exp2((state[p][0] - top) * c)
            total = total + state[p][1] * factor
            acc = acc + state[p][2] * factor
        state[p] = (top, total, acc)

    def own(p, kp):
        attend(p, rcv[1, pl.ds(kp * half, half), :], rcv[2, pl.ds(kp * half, half), :])

    def side(p, kp):
        attend(p, kvx[0, pl.ds(kp * half, half), :], kvx[1, pl.ds(kp * half, half), :])

    c_copies = {}

    def finish(p):
        _, total, acc = state[p]
        o = acc / total
        o = o[:half] - lam * o[half:]
        meansq = jnp.mean(o * o, axis=1, keepdims=True)
        normed = (o * lax.rsqrt(meansq + 1e-06) * gain).astype(BF16)
        normed = normed.reshape(2, nh, rows, vd)
        for d in range(1, nh):
            nsnd[p, d - 1] = normed[:, d]
            c_copies[p, d] = remote(
                nsnd.at[p, d - 1], nrm.at[p, h], c_ss.at[p, d - 1], c_rs.at[p, d - 1], head_peer(nh - d)
            )
            c_copies[p, d].start()
        nrm[p, h] = normed[:, 0]

    def arrived(copies, p):
        for (cp, d), copy in copies.items():
            if cp == p:
                copy.wait_recv()

    pl.semaphore_wait(barrier, len(peers))
    to_row = remote(tok_ref, tok.at[1], a_ss.at[1], a_rs.at[1], row_peer)
    to_row.start()
    to_core = remote(tok_ref, tok.at[0], a_ss.at[0], a_rs.at[0], core_peer)
    to_core.start()
    forward = remote(tok.at[1], tok.at[2], a_ss.at[2], a_rs.at[2], core_peer)
    pending += [to_row, to_core, forward]
    project(0, tok_ref[...])
    send_kv(0)
    send_q(0)
    to_core.wait_recv()
    project(1, tok[0])
    send_kv(1)
    send_q(1)
    to_row.wait_recv()
    forward.start()
    project(2, tok[1])
    send_kv(2)
    forward.wait_recv()
    project(3, tok[2])
    send_kv(3)
    send_q(2)
    send_q(3)
    relay(0)
    relay(1)
    for u in range(2):
        arrived(q_copies, u)
    own(0, 0)
    relay(2)
    for u in range(2):
        arrived(x_copies, u)
    side(0, 0)
    relay(3)
    own(0, 1)
    for u in range(2, 4):
        arrived(q_copies, u)
    own(1, 0)
    side(1, 0)
    own(1, 1)
    for u in range(2, 4):
        arrived(x_copies, u)
    side(1, 1)
    finish(1)
    side(0, 1)
    finish(0)

    step = width // CHUNKS
    d_copies, y_copies = {}, []

    def out_part(p):
        arrived(c_copies, p)
        n = jnp.concatenate([nrm[p, i].reshape(pair, vd) for i in range(nh)], axis=1)
        for k in range(CHUNKS):
            part = jnp.dot(n, wo[:, k * step : (k + 1) * step], preferred_element_type=F32)
            dsnd[p, k] = part[rows:].astype(BF16)
            keep[p, k] = part[:rows]
            d_copies[p, k] = remote(dsnd.at[p, k], drcv.at[p, k], d_ss.at[p, k], d_rs.at[p, k], core_peer)
            d_copies[p, k].start()

    loads[3].wait()
    out_part(1)
    for k in range(CHUNKS):
        d_copies[1, k].wait_recv()
        ysnd[k] = (keep[1, k] + drcv[1, k].astype(F32)).astype(BF16)
        y_copies.append(remote(ysnd.at[k], yrcv.at[k], y_ss.at[k], y_rs.at[k], row_peer))
        y_copies[k].start()
    out_part(0)
    for k in range(CHUNKS):
        d_copies[0, k].wait_recv()
        y_copies[k].wait_recv()
        whole = keep[0, k] + drcv[0, k].astype(F32) + yrcv[k].astype(F32)
        out_ref[:, k * step : (k + 1) * step] = whole.astype(BF16)
    for copies in (z_copies, q_copies, x_copies, c_copies, d_copies):
        pending += list(copies.values())
    for copy in pending + y_copies:
        copy.wait_send()


def fused(tokens, w_query, w_key, w_value, w_out, mix_weight, out_gain):
    rows, width = tokens.shape
    nh = mix_weight.shape[0]
    vd = out_gain.shape[0]
    cols = w_query.shape[1]
    block = 4 * rows
    step = width // CHUNKS
    vmem, hbm = pl.BlockSpec(memory_space=pltpu.VMEM), pl.BlockSpec(memory_space=pl.ANY)
    dma = pltpu.SemaphoreType.DMA
    return pl.pallas_call(
        functools.partial(kernel, nh),
        out_shape=jax.ShapeDtypeStruct((rows, width), BF16),
        in_specs=[pl.BlockSpec(memory_space=pltpu.SMEM), vmem, vmem, hbm, hbm, hbm, hbm],
        out_specs=vmem,
        scratch_shapes=[
            pltpu.VMEM((width, cols), BF16),
            pltpu.VMEM((width, cols), BF16),
            pltpu.VMEM((width, cols), BF16),
            pltpu.VMEM(w_out.shape, BF16),
            pltpu.VMEM((3, rows, width), BF16),
            pltpu.VMEM((nh, 3, block, vd), BF16),
            pltpu.VMEM((3, nh * block, vd), BF16),
            pltpu.VMEM((2, nh * block, vd), BF16),
            pltpu.VMEM((2, nh - 1, 2, rows, vd), BF16),
            pltpu.VMEM((2, nh, 2, rows, vd), BF16),
            pltpu.VMEM((2, CHUNKS, rows, step), F32),
            pltpu.VMEM((2, CHUNKS, rows, step), BF16),
            pltpu.VMEM((2, CHUNKS, rows, step), BF16),
            pltpu.VMEM((CHUNKS, rows, step), BF16),
            pltpu.VMEM((CHUNKS, rows, step), BF16),
            dma((4,)), dma((3,)), dma((3,)),
            dma((2, 4, nh - 1)), dma((2, 4, nh - 1)), dma((4, nh)), dma((4, nh)),
            dma((2, nh - 1)), dma((2, nh - 1)),
            dma((2, CHUNKS)), dma((2, CHUNKS)), dma((CHUNKS,)), dma((CHUNKS,)),
        ],
        compiler_params=pltpu.CompilerParams(
            collective_id=0, has_side_effects=True, vmem_limit_bytes=56 * 2**20
        ),
    )(mix_weight, out_gain.reshape(1, vd), tokens, w_query, w_key, w_value, w_out)


def pick(mesh, *arrays):
    tokens, w_query, _, _, _, mix_weight, out_gain = arrays
    nh = mix_weight.shape[0]
    fits = (
        mesh.shape["sp"] == 2 * nh
        and mesh.shape["tp"] == 4
        and w_query.shape[1] == nh * out_gain.shape[0]
        and out_gain.shape[0] == 128
        and tokens.shape[0] % 16 == 0
        and tokens.shape[1] % (128 * CHUNKS) == 0
    )
    return fused(*arrays) if fits else shards(*arrays)


def solution(mesh):
    in_specs = (
        P(("sp", "tp"), None),
        P(None, "tp"),
        P(None, "tp"),
        P(None, "tp"),
        P("tp", None),
        P("tp"),
        P(),
    )
    out_specs = P(("sp", "tp"), None)
    return jax.shard_map(functools.partial(pick, mesh), mesh=mesh, in_specs=in_specs, out_specs=out_specs, check_vma=False)
```
